32 devices in a mesh: row: 8 (over z, y), col: 4 (over x, core).
Axes of the slice: x: 2, y: 2, z: 4, core: 2. Of those that a mesh axis runs over, the one named last changes fastest.
Arguments:
- tokens: bfloat16 [2, 32, 16, 2048], P(None, 'row', 'col'), may hold values from -6 to 6
- norm_gain: bfloat16 [2048], replicated, may hold values from 0.099609375 to 1.8984375
- w_mix_in: bfloat16 [2048, 1024], replicated, may hold values from -0.125 to 0.125
- w_mix_out: bfloat16 [1024, 2048], replicated, may hold values from -0.1875 to 0.1875
Outputs:
- mixed_tokens: bfloat16 [2, 16, 32, 2048], P(None, 'row', 'col')
The draws below stay inside these ranges and needn't reach their ends.
All inputs are finite; a program needn't handle non-finite values.
Results may differ from the reference program's by a relative error of at most 0.013.
Values may be sent and summed in bfloat16 or wider, within the bound.
A program may use at most 64 MiB of HBM per device.

```python
import jax
import jax.numpy as jnp
from jax import lax

D = 2048
F = 1024
G = 128
SEQS = 2
LEN_ROW = 32
LEN_COL = 16


def block_scale(own_key, shape, cuts, low, largest):
    def one(position, shards_of):
        heights = jax.random.uniform(jax.random.fold_in(jax.random.fold_in(own_key, 6), position), (shards_of,), jnp.float32, low / len(cuts), largest / len(cuts))
        return jnp.repeat(jnp.exp(heights), shape[position] // shards_of).reshape((-1,) + (1,) * (len(shape) - position - 1))

    level = one(*cuts[0])
    for cut in cuts[1:]:
        level = level * one(*cut)
    return level


def gaussian(key, extent, width, limit, cuts=(), kind=jnp.bfloat16):
    array = width * jax.random.normal(key, extent, jnp.float32)
    if cuts:
        array = array * block_scale(key, extent, cuts, -0.22, 0.18)
    return jnp.clip(array, -limit, limit).astype(kind)


def setup_inputs(seed: int = 0) -> dict:
    streams_of = jax.random.split(jax.random.key(seed), 5)
    return {
        "tokens": gaussian(streams_of[0], (SEQS, LEN_ROW, LEN_COL, D), 1.0, 6.0, ((1, 8), (2, 4))),
        "norm_gain": jnp.clip(1.0 + 0.18 * jax.random.normal(streams_of[1], (D,), jnp.float32), 0.099609375, 1.8984375).astype(jnp.bfloat16),
        "w_mix_in": gaussian(streams_of[2], (D, F), D ** -0.5, 0.125),
        "w_mix_out": gaussian(streams_of[3], (F, D), F ** -0.5, 0.1875),
    }


EPS = 1e-06

def reference(tokens, norm_gain, w_mix_in, w_mix_out):

    def one_sequence(sequence):
        scaled = sequence.astype(jnp.float32)
        mean_square = lax.optimization_barrier(jnp.mean(scaled * scaled, axis=-1, keepdims=True))
        normed = (scaled * lax.rsqrt(mean_square + EPS) * norm_gain.astype(jnp.float32)).astype(jnp.bfloat16)
        mixing_in = jnp.dot(normed.reshape(LEN_ROW * LEN_COL, D), w_mix_in, preferred_element_type=jnp.float32).astype(jnp.bfloat16)
        grouped = mixing_in.astype(jnp.float32).reshape(LEN_ROW * LEN_COL, F // G, G)
        spectrum = jnp.fft.fft2(grouped, axes=(0, 2), norm='ortho').real
        mixed = spectrum.astype(jnp.bfloat16).reshape(LEN_COL * LEN_ROW, F)
        output = jnp.dot(mixed, w_mix_out, preferred_element_type=jnp.float32).astype(jnp.bfloat16)
        return output.reshape(LEN_COL, LEN_ROW, D)
    return lax.map(one_sequence, tokens)
```

```python
import functools
import math

import jax
import jax.numpy as jnp
import numpy as np
from jax import lax
from jax.experimental import pallas as pl
from jax.experimental.pallas import tpu as pltpu
from jax.sharding import PartitionSpec as P

MESH = pl.DeviceIdType.MESH

G = 128


EPS = 1e-06
HIGHEST = lax.Precision.HIGHEST


def as_sent(x):

    def short(part):
        return part.astype(jnp.bfloat16) if part.dtype == jnp.float32 else part

    return jax.tree.map(short, x)


def phase_table(count_first, count_second, period, first_start):
    first_index = lax.iota(jnp.int32, count_first) + first_start
    second_index = lax.iota(jnp.int32, count_second)
    turn_count = first_index[:, None] * second_index[None, :] % period
    phases = turn_count.astype(jnp.float32) * (2.0 * math.pi / period)
    return (jnp.cos(phases), jnp.sin(phases))


def packed_table(group_width):
    source = lax.iota(jnp.int32, group_width)
    column = lax.iota(jnp.int32, group_width)
    pair_index = column // 2
    frequency = jnp.where(column == 1, group_width // 2, pair_index)
    use_sine = (column % 2 == 1) & (pair_index > 0)
    turn_count = source[:, None] * frequency[None, :] % group_width
    phases = turn_count.astype(jnp.float32) * (2.0 * math.pi / group_width)
    return jnp.where(use_sine[None, :], jnp.sin(phases), jnp.cos(phases)) / math.sqrt(group_width)


def staged_body(tokens, norm_gain, w_mix_in, w_mix_out):
    seq_count, rows_here, cols_here, width = tokens.shape
    row_devices = lax.axis_size("row")
    col_devices = lax.axis_size("col")
    len_first = rows_here * row_devices
    len_second = cols_here * col_devices
    seq_length = len_first * len_second
    features = w_mix_in.shape[1]
    share = features // row_devices
    groups = features // G
    scaled = tokens.astype(jnp.float32)
    mean_square = jnp.mean(scaled * scaled, axis=-1, keepdims=True)
    normed = (scaled * lax.rsqrt(mean_square + EPS) * norm_gain.astype(jnp.float32)).astype(
        jnp.bfloat16
    )
    mixing_in = jnp.dot(
        normed.reshape(-1, width), w_mix_in, preferred_element_type=jnp.float32
    ).astype(jnp.bfloat16)
    grouped = mixing_in.astype(jnp.float32).reshape(seq_count, rows_here, cols_here, groups, G)
    first_cos, first_sin = phase_table(len_first, len_first, len_first, 0)
    first_cos = first_cos / math.sqrt(len_first)
    first_sin = first_sin / math.sqrt(len_first)
    col_start = lax.axis_index("col") * cols_here
    twist_cos, twist_sin = phase_table(cols_here, len_first, seq_length, col_start)
    twist_cos = twist_cos[None, :, None, :]
    twist_sin = twist_sin[None, :, None, :]
    packed = jnp.einsum("sabgc,cm->sabgm", grouped, packed_table(G), precision=HIGHEST)
    packed = packed.reshape(seq_count, rows_here, cols_here, features)
    turned = jnp.transpose(
        lax.all_to_all(
            packed.astype(jnp.bfloat16), "row", split_axis=3, concat_axis=1, tiled=True
        ).astype(packed.dtype),
        (0, 2, 3, 1),
    )
    real_out = jnp.einsum("njft,tk->njfk", turned, first_cos, precision=HIGHEST)
    imag_out = -jnp.einsum("njft,tk->njfk", turned, first_sin, precision=HIGHEST)
    spec_real = real_out * twist_cos + imag_out * twist_sin
    spec_imag = imag_out * twist_cos - real_out * twist_sin
    second_cos, second_sin = phase_table(len_second, len_second, len_second, 0)
    second_cos = second_cos / math.sqrt(len_second)
    second_sin = second_sin / math.sqrt(len_second)
    row_start = lax.axis_index("row") * share
    pair_global = row_start // 2 + lax.iota(jnp.int32, share // 2)
    head_pair = (pair_global % (G // 2) == 0)[:, None]
    real_in = lax.all_to_all(
        as_sent(spec_real), "col", split_axis=3, concat_axis=1, tiled=True
    ).astype(spec_real.dtype)
    imag_in = lax.all_to_all(
        as_sent(spec_imag), "col", split_axis=3, concat_axis=1, tiled=True
    ).astype(spec_imag.dtype)
    real_turned = jnp.transpose(real_in, (0, 3, 2, 1))
    imag_turned = jnp.transpose(imag_in, (0, 3, 2, 1))
    real_out = jnp.einsum("nqft,tk->nqfk", real_turned, second_cos, precision=HIGHEST) + jnp.einsum(
        "nqft,tk->nqfk", imag_turned, second_sin, precision=HIGHEST
    )
    imag_out = jnp.einsum("nqft,tk->nqfk", imag_turned, second_cos, precision=HIGHEST) - jnp.einsum(
        "nqft,tk->nqfk", real_turned, second_sin, precision=HIGHEST
    )
    out_shape = real_out.shape
    pair_shape = out_shape[:2] + (share // 2, 2, out_shape[3])
    real_pairs = real_out.reshape(pair_shape)
    imag_pairs = imag_out.reshape(pair_shape)
    even_real = real_pairs[:, :, :, 0, :]
    odd_real = real_pairs[:, :, :, 1, :]
    odd_imag = imag_pairs[:, :, :, 1, :]
    low_freq = jnp.where(head_pair, even_real, even_real + odd_imag)
    high_freq = jnp.where(head_pair, odd_real, even_real - odd_imag)
    joined = jnp.stack([low_freq, high_freq], axis=3).reshape(out_shape).astype(jnp.bfloat16)
    mixed = jnp.transpose(joined, (0, 3, 1, 2))
    piece = lax.all_to_all(mixed, "row", split_axis=1, concat_axis=3, tiled=True)
    paired = piece.reshape(piece.shape[:-1] + (groups, G // 2, 2))
    low_freq = paired[..., 0]
    high_freq = paired[..., 1]
    natural = jnp.concatenate(
        [low_freq, high_freq[..., :1], jnp.flip(high_freq[..., 1:], axis=-1)], axis=-1
    )
    project_piece = natural.reshape(piece.shape)
    flat = project_piece.reshape(-1, features)
    output = jnp.dot(flat, w_mix_out, preferred_element_type=jnp.float32).astype(jnp.bfloat16)
    return output.reshape(project_piece.shape[:-1] + (width,))


class Plan:
    def __init__(self, mesh, tokens_shape, features):
        self.rows, self.cols = mesh.shape["row"], mesh.shape["col"]
        self.devices = self.rows * self.cols
        self.seqs, len_first, len_second, self.width = tokens_shape
        self.len_first, self.len_second = len_first, len_second
        self.features = features
        self.groups = features // G
        self.units = self.seqs * self.groups
        self.t1, self.t2 = len_first // self.rows, len_second // self.cols
        self.here = self.t1 * self.t2
        self.length = len_first * len_second
        self.q2, self.q1 = len_second // self.rows, len_first // self.cols

    def fits(self):
        if self.features % G or self.devices % self.units or self.length > 1024:
            return False
        if self.len_second % self.rows or self.len_first % self.cols:
            return False
        self.halves = self.devices // self.units
        if self.rows % self.halves or self.here % 16 or self.q1 % 8:
            return False
        self.half_rows = self.rows // self.halves
        return True

    def tables(self):
        row, col, a, b = np.meshgrid(
            np.arange(self.rows), np.arange(self.cols), np.arange(self.t1), np.arange(self.t2), indexing="ij"
        )
        time = ((row * self.t1 + a) * self.len_second + col * self.t2 + b).reshape(-1)
        row, col, a, b = np.meshgrid(
            np.arange(self.rows), np.arange(self.cols), np.arange(self.q2), np.arange(self.q1), indexing="ij"
        )
        freq = (col * self.q1 + b + self.len_first * (row * self.q2 + a)).reshape(self.halves, -1)
        turn = 2.0 * np.pi / self.length * (freq[:, :, None] * time[None, None, :] % self.length)
        scale = 1.0 / math.sqrt(self.length * G)
        first = 2.0 ** round(math.log2(scale) / 2)
        position = np.concatenate([np.cos(turn), np.sin(turn)], axis=1) * first
        channel = np.arange(G)
        turn = 2.0 * np.pi / G * (channel[:, None] * channel[None, :] % G)
        channel = np.concatenate([np.cos(turn), -np.sin(turn)], axis=0) * (scale / first)
        return jnp.asarray(position, jnp.bfloat16), jnp.asarray(channel, jnp.bfloat16)


VMEM_BYTES = 67043328
IN_CHUNKS = 4
OUT_CHUNKS = 4


def mix_kernel(
    plan, tokens_hbm, gain_hbm, w_in_hbm, w_out_hbm, table_hbm, channel_hbm, out_ref,
    tokens_v, gain_v, w_in_v, w_out_v, table_v, channel_v, flat_v,
    x_send, x_recv, s_send, s_recv,
    load_sem, in_sem, out_sem, x_send_sem, x_recv_sem, s_send_sem, s_recv_sem,
):
    row, col = lax.axis_index("row"), lax.axis_index("col")
    me = row * plan.cols + col
    half = row // plan.half_rows
    unit = lax.rem(me, plan.units)
    place = lambda d: {"row": d // plan.cols, "col": lax.rem(d, plan.cols)}

    barrier = pltpu.get_barrier_semaphore()

    def greet(i, carry):
        pl.semaphore_signal(
            barrier, inc=1, device_id=place(lax.rem(me + i, plan.devices)), device_id_type=MESH
        )
        return carry

    token_load = pltpu.make_async_copy(tokens_hbm, tokens_v, load_sem.at[0])
    gain_load = pltpu.make_async_copy(gain_hbm, gain_v, load_sem.at[1])
    table_load = pltpu.make_async_copy(table_hbm.at[half], table_v, load_sem.at[2])
    channel_load = pltpu.make_async_copy(channel_hbm, channel_v, load_sem.at[3])
    depth = plan.width // IN_CHUNKS
    in_loads = [
        pltpu.make_async_copy(
            w_in_hbm.at[pl.ds(j * depth, depth)], w_in_v.at[pl.ds(j * depth, depth)], in_sem.at[j]
        )
        for j in range(IN_CHUNKS)
    ]
    span = plan.width // OUT_CHUNKS
    out_load = pltpu.make_async_copy(w_out_hbm, w_out_v, out_sem.at[0])
    token_load.start()
    gain_load.start()
    for load in in_loads:
        load.start()
    table_load.start()
    channel_load.start()
    out_load.start()
    lax.fori_loop(1, plan.devices, greet, 0)

    token_load.wait()
    for s in range(plan.seqs):
        for a in range(plan.t1):
            flat_v[pl.ds((s * plan.t1 + a) * plan.t2, plan.t2), :] = tokens_v[s, a].astype(jnp.float32)
    scaled = flat_v[...]
    mean_square = jnp.mean(scaled * scaled, axis=-1, keepdims=True)
    gain_load.wait()
    gain = gain_v[...].astype(jnp.float32).reshape(1, plan.width)
    normed = (scaled * lax.rsqrt(mean_square + EPS) * gain).astype(jnp.bfloat16)
    mixing = None
    for j in range(IN_CHUNKS):
        in_loads[j].wait()
        part = jnp.dot(
            normed[:, j * depth : (j + 1) * depth],
            w_in_v[pl.ds(j * depth, depth), :],
            preferred_element_type=jnp.float32,
        )
        mixing = part if mixing is None else mixing + part
    mixing = mixing.astype(jnp.bfloat16)
    for g in range(plan.groups):
        for s in range(plan.seqs):
            x_send[g * plan.seqs + s] = mixing[s * plan.here : (s + 1) * plan.here, g * G : (g + 1) * G]

    pl.semaphore_wait(barrier, plan.devices - 1)

    def x_copy(source, target):
        return pltpu.make_async_remote_copy(
            src_ref=x_send.at[lax.rem(target, plan.units)],
            dst_ref=x_recv.at[source],
            send_sem=x_send_sem.at[target],
            recv_sem=x_recv_sem.at[source],
            device_id=place(target),
            device_id_type=MESH,
        )

    def x_start(i, carry):
        x_copy(me, lax.rem(me + i, plan.devices)).start()
        return carry

    lax.fori_loop(1, plan.devices, x_start, 0)
    x_recv[me] = x_send[unit]
    table_load.wait()
    channel_load.wait()

    def x_wait(i, carry):
        x_copy(lax.rem(me + i, plan.devices), me).wait_recv()
        return carry

    lax.fori_loop(1, plan.devices, x_wait, 0)
    values = x_recv[...].reshape(plan.length, G)
    turned = jnp.dot(table_v[...], values, preferred_element_type=jnp.float32).astype(jnp.bfloat16)
    owned = plan.length // plan.halves
    both = jnp.concatenate([turned[:owned], turned[owned:]], axis=1)
    spectrum = jnp.dot(both, channel_v[...], preferred_element_type=jnp.float32).astype(jnp.bfloat16)
    s_send[...] = spectrum.reshape(s_send.shape)

    def s_copy(source, target):
        return pltpu.make_async_remote_copy(
            src_ref=s_send.at[target],
            dst_ref=s_recv.at[source],
            send_sem=s_send_sem.at[target],
            recv_sem=s_recv_sem.at[source],
            device_id=place(half * plan.units + target),
            device_id_type=MESH,
        )

    def s_start(i, carry):
        s_copy(unit, lax.rem(unit + i, plan.units)).start()
        return carry

    lax.fori_loop(1, plan.units, s_start, 0)
    s_recv[unit] = s_send[unit]
    out_load.wait()

    def s_wait(i, carry):
        s_copy(lax.rem(unit + i, plan.units), unit).wait_recv()
        return carry

    lax.fori_loop(1, plan.units, s_wait, 0)
    mixed = jnp.concatenate(
        [
            jnp.concatenate([s_recv[g * plan.seqs + s] for s in range(plan.seqs)], axis=0)
            for g in range(plan.groups)
        ],
        axis=1,
    )
    for j in range(OUT_CHUNKS):
        piece = jnp.dot(
            mixed, w_out_v[:, pl.ds(j * span, span)], preferred_element_type=jnp.float32
        )
        for s in range(plan.seqs):
            for q in range(plan.q2):
                start = (s * plan.q2 + q) * plan.q1
                out_ref[s, q, :, pl.ds(j * span, span)] = piece[start : start + plan.q1].astype(jnp.bfloat16)

    def x_sent(i, carry):
        x_copy(me, lax.rem(me + i, plan.devices)).wait_send()
        return carry

    def s_sent(i, carry):
        s_copy(unit, lax.rem(unit + i, plan.units)).wait_send()
        return carry

    lax.fori_loop(1, plan.devices, x_sent, 0)
    lax.fori_loop(1, plan.units, s_sent, 0)


def kernel_body(plan, tokens, norm_gain, w_mix_in, w_mix_out):
    table, channel = plan.tables()
    bf16 = jnp.bfloat16
    dma = pltpu.SemaphoreType.DMA
    return pl.pallas_call(
        functools.partial(mix_kernel, plan),
        out_shape=jax.ShapeDtypeStruct((plan.seqs, plan.q2, plan.q1, plan.width), bf16),
        in_specs=[pl.BlockSpec(memory_space=pl.ANY)] * 6,
        out_specs=pl.BlockSpec(memory_space=pltpu.VMEM),
        scratch_shapes=[
            pltpu.VMEM(tokens.shape, bf16),
            pltpu.VMEM(norm_gain.shape, bf16),
            pltpu.VMEM(w_mix_in.shape, bf16),
            pltpu.VMEM(w_mix_out.shape, bf16),
            pltpu.VMEM(table.shape[1:], bf16),
            pltpu.VMEM(channel.shape, bf16),
            pltpu.VMEM((plan.seqs * plan.here, plan.width), jnp.float32),
            pltpu.VMEM((plan.units, plan.here, G), bf16),
            pltpu.VMEM((plan.devices, plan.here, G), bf16),
            pltpu.VMEM((plan.units, plan.q2 * plan.q1, G), bf16),
            pltpu.VMEM((plan.units, plan.q2 * plan.q1, G), bf16),
            dma((4,)),
            dma((IN_CHUNKS,)),
            dma((OUT_CHUNKS,)),
            dma((plan.devices,)),
            dma((plan.devices,)),
            dma((plan.units,)),
            dma((plan.units,)),
        ],
        compiler_params=pltpu.CompilerParams(
            collective_id=0, has_side_effects=True, vmem_limit_bytes=VMEM_BYTES
        ),
    )(tokens, norm_gain, w_mix_in, w_mix_out, table, channel)


def solution(mesh):
    placed = (P(None, "row", "col", None), P(), P(), P())

    def run(tokens, norm_gain, w_mix_in, w_mix_out):
        plan = Plan(mesh, tokens.shape, w_mix_in.shape[1])
        body = functools.partial(kernel_body, plan) if plan.fits() else staged_body
        return jax.shard_map(
            body, mesh=mesh, in_specs=placed, out_specs=P(None, "row", "col", None), check_vma=False
        )(tokens, norm_gain, w_mix_in, w_mix_out)

    return run
```

```python
import functools
import math

import jax
import jax.numpy as jnp
import numpy as np
from jax import lax
from jax.experimental import pallas as pl
from jax.experimental.pallas import tpu as pltpu
from jax.sharding import PartitionSpec as P

MESH = pl.DeviceIdType.MESH

G = 128


EPS = 1e-06
HIGHEST = lax.Precision.HIGHEST


def as_sent(x):

    def short(part):
        return part.astype(jnp.bfloat16) if part.dtype == jnp.float32 else part

    return jax.tree.map(short, x)


def phase_table(count_first, count_second, period, first_start):
    first_index = lax.iota(jnp.int32, count_first) + first_start
    second_index = lax.iota(jnp.int32, count_second)
    turn_count = first_index[:, None] * second_index[None, :] % period
    phases = turn_count.astype(jnp.float32) * (2.0 * math.pi / period)
    return (jnp.cos(phases), jnp.sin(phases))


def packed_table(group_width):
    source = lax.iota(jnp.int32, group_width)
    column = lax.iota(jnp.int32, group_width)
    pair_index = column // 2
    frequency = jnp.where(column == 1, group_width // 2, pair_index)
    use_sine = (column % 2 == 1) & (pair_index > 0)
    turn_count = source[:, None] * frequency[None, :] % group_width
    phases = turn_count.astype(jnp.float32) * (2.0 * math.pi / group_width)
    return jnp.where(use_sine[None, :], jnp.sin(phases), jnp.cos(phases)) / math.sqrt(group_width)


def staged_body(tokens, norm_gain, w_mix_in, w_mix_out):
    seq_count, rows_here, cols_here, width = tokens.shape
    row_devices = lax.axis_size("row")
    col_devices = lax.axis_size("col")
    len_first = rows_here * row_devices
    len_second = cols_here * col_devices
    seq_length = len_first * len_second
    features = w_mix_in.shape[1]
    share = features // row_devices
    groups = features // G
    scaled = tokens.astype(jnp.float32)
    mean_square = jnp.mean(scaled * scaled, axis=-1, keepdims=True)
    normed = (scaled * lax.rsqrt(mean_square + EPS) * norm_gain.astype(jnp.float32)).astype(
        jnp.bfloat16
    )
    mixing_in = jnp.dot(
        normed.reshape(-1, width), w_mix_in, preferred_element_type=jnp.float32
    ).astype(jnp.bfloat16)
    grouped = mixing_in.astype(jnp.float32).reshape(seq_count, rows_here, cols_here, groups, G)
    first_cos, first_sin = phase_table(len_first, len_first, len_first, 0)
    first_cos = first_cos / math.sqrt(len_first)
    first_sin = first_sin / math.sqrt(len_first)
    col_start = lax.axis_index("col") * cols_here
    twist_cos, twist_sin = phase_table(cols_here, len_first, seq_length, col_start)
    twist_cos = twist_cos[None, :, None, :]
    twist_sin = twist_sin[None, :, None, :]
    packed = jnp.einsum("sabgc,cm->sabgm", grouped, packed_table(G), precision=HIGHEST)
    packed = packed.reshape(seq_count, rows_here, cols_here, features)
    turned = jnp.transpose(
        lax.all_to_all(
            packed.astype(jnp.bfloat16), "row", split_axis=3, concat_axis=1, tiled=True
        ).astype(packed.dtype),
        (0, 2, 3, 1),
    )
    real_out = jnp.einsum("njft,tk->njfk", turned, first_cos, precision=HIGHEST)
    imag_out = -jnp.einsum("njft,tk->njfk", turned, first_sin, precision=HIGHEST)
    spec_real = real_out * twist_cos + imag_out * twist_sin
    spec_imag = imag_out * twist_cos - real_out * twist_sin
    second_cos, second_sin = phase_table(len_second, len_second, len_second, 0)
    second_cos = second_cos / math.sqrt(len_second)
    second_sin = second_sin / math.sqrt(len_second)
    row_start = lax.axis_index("row") * share
    pair_global = row_start // 2 + lax.iota(jnp.int32, share // 2)
    head_pair = (pair_global % (G // 2) == 0)[:, None]
    real_in = lax.all_to_all(
        as_sent(spec_real), "col", split_axis=3, concat_axis=1, tiled=True
    ).astype(spec_real.dtype)
    imag_in = lax.all_to_all(
        as_sent(spec_imag), "col", split_axis=3, concat_axis=1, tiled=True
    ).astype(spec_imag.dtype)
    real_turned = jnp.transpose(real_in, (0, 3, 2, 1))
    imag_turned = jnp.transpose(imag_in, (0, 3, 2, 1))
    real_out = jnp.einsum("nqft,tk->nqfk", real_turned, second_cos, precision=HIGHEST) + jnp.einsum(
        "nqft,tk->nqfk", imag_turned, second_sin, precision=HIGHEST
    )
    imag_out = jnp.einsum("nqft,tk->nqfk", imag_turned, second_cos, precision=HIGHEST) - jnp.einsum(
        "nqft,tk->nqfk", real_turned, second_sin, precision=HIGHEST
    )
    out_shape = real_out.shape
    pair_shape = out_shape[:2] + (share // 2, 2, out_shape[3])
    real_pairs = real_out.reshape(pair_shape)
    imag_pairs = imag_out.reshape(pair_shape)
    even_real = real_pairs[:, :, :, 0, :]
    odd_real = real_pairs[:, :, :, 1, :]
    odd_imag = imag_pairs[:, :, :, 1, :]
    low_freq = jnp.where(head_pair, even_real, even_real + odd_imag)
    high_freq = jnp.where(head_pair, odd_real, even_real - odd_imag)
    joined = jnp.stack([low_freq, high_freq], axis=3).reshape(out_shape).astype(jnp.bfloat16)
    mixed = jnp.transpose(joined, (0, 3, 1, 2))
    piece = lax.all_to_all(mixed, "row", split_axis=1, concat_axis=3, tiled=True)
    paired = piece.reshape(piece.shape[:-1] + (groups, G // 2, 2))
    low_freq = paired[..., 0]
    high_freq = paired[..., 1]
    natural = jnp.concatenate(
        [low_freq, high_freq[..., :1], jnp.flip(high_freq[..., 1:], axis=-1)], axis=-1
    )
    project_piece = natural.reshape(piece.shape)
    flat = project_piece.reshape(-1, features)
    output = jnp.dot(flat, w_mix_out, preferred_element_type=jnp.float32).astype(jnp.bfloat16)
    return output.reshape(project_piece.shape[:-1] + (width,))


class Plan:
    def __init__(self, mesh, tokens_shape, features):
        self.rows, self.cols = mesh.shape["row"], mesh.shape["col"]
        self.devices = self.rows * self.cols
        self.seqs, len_first, len_second, self.width = tokens_shape
        self.len_first, self.len_second = len_first, len_second
        self.features = features
        self.groups = features // G
        self.units = self.seqs * self.groups
        self.t1, self.t2 = len_first // self.rows, len_second // self.cols
        self.here = self.t1 * self.t2
        self.length = len_first * len_second
        self.q2, self.q1 = len_second // self.rows, len_first // self.cols

    def fits(self):
        if self.features % G or self.devices % self.units or self.length > 1024:
            return False
        if self.devices & (self.devices - 1) or self.units & (self.units - 1):
            return False
        if self.len_second % self.rows or self.len_first % self.cols:
            return False
        self.halves = self.devices // self.units
        if self.rows % self.halves or self.here % 16 or self.q1 % 8:
            return False
        self.half_rows = self.rows // self.halves
        return True

    def tables(self):
        row, col, a, b = np.meshgrid(
            np.arange(self.rows), np.arange(self.cols), np.arange(self.t1), np.arange(self.t2), indexing="ij"
        )
        time = ((row * self.t1 + a) * self.len_second + col * self.t2 + b).reshape(-1)
        row, col, a, b = np.meshgrid(
            np.arange(self.rows), np.arange(self.cols), np.arange(self.q2), np.arange(self.q1), indexing="ij"
        )
        freq = (col * self.q1 + b + self.len_first * (row * self.q2 + a)).reshape(self.halves, -1)
        turn = 2.0 * np.pi / self.length * (freq[:, :, None] * time[None, None, :] % self.length)
        scale = 1.0 / math.sqrt(self.length * G)
        first = 2.0 ** round(math.log2(scale) / 2)
        position = np.concatenate([np.cos(turn), np.sin(turn)], axis=1) * first
        channel = np.arange(G)
        turn = 2.0 * np.pi / G * (channel[:, None] * channel[None, :] % G)
        channel = np.concatenate([np.cos(turn), -np.sin(turn)], axis=0) * (scale / first)
        return jnp.asarray(position, jnp.bfloat16), jnp.asarray(channel, jnp.bfloat16)


VMEM_BYTES = 16 * 1024 * 1024
IN_CHUNKS = 4
OUT_CHUNKS = 4


def mix_kernel(
    plan, tokens_hbm, gain_hbm, w_in_hbm, w_out_hbm, table_hbm, channel_hbm, out_ref,
    tokens_v, gain_v, w_in_v, w_out_v, table_v, channel_v, flat_v,
    x_send, x_recv, s_send, s_recv,
    load_sem, in_sem, out_sem, x_send_sem, x_recv_sem, s_send_sem, s_recv_sem,
):
    row, col = lax.axis_index("row"), lax.axis_index("col")
    me = row * plan.cols + col
    half = row // plan.half_rows
    unit = lax.rem(me, plan.units)
    place = lambda d: {"row": d // plan.cols, "col": lax.rem(d, plan.cols)}

    barrier = pltpu.get_barrier_semaphore()

    flips = []
    bit = 1
    while bit < plan.devices:
        flips.append((bit, bit * (1 - 2 * lax.rem(me // bit, 2))))
        bit *= 2

    def partner(mask):
        return me + sum(step for bit, step in flips if mask & bit)

    token_load = pltpu.make_async_copy(tokens_hbm, tokens_v, load_sem.at[0])
    gain_load = pltpu.make_async_copy(gain_hbm, gain_v, load_sem.at[1])
    table_load = pltpu.make_async_copy(table_hbm.at[half], table_v, load_sem.at[2])
    channel_load = pltpu.make_async_copy(channel_hbm, channel_v, load_sem.at[3])
    depth = plan.width // IN_CHUNKS
    in_loads = [
        pltpu.make_async_copy(
            w_in_hbm.at[pl.ds(j * depth, depth)], w_in_v.at[pl.ds(j * depth, depth)], in_sem.at[j]
        )
        for j in range(IN_CHUNKS)
    ]
    span = plan.width // OUT_CHUNKS
    out_load = pltpu.make_async_copy(w_out_hbm, w_out_v, out_sem.at[0])
    token_load.start()
    gain_load.start()
    for load in in_loads:
        load.start()
    table_load.start()
    channel_load.start()
    out_load.start()
    for mask in range(plan.devices - 1, 0, -1):
        pl.semaphore_signal(barrier, inc=1, device_id=place(partner(mask)), device_id_type=MESH)

    token_load.wait()
    for s in range(plan.seqs):
        for a in range(plan.t1):
            flat_v[pl.ds((s * plan.t1 + a) * plan.t2, plan.t2), :] = tokens_v[s, a].astype(jnp.float32)
    scaled = flat_v[...]
    mean_square = jnp.mean(scaled * scaled, axis=-1, keepdims=True)
    gain_load.wait()
    gain = gain_v[...].astype(jnp.float32).reshape(1, plan.width)
    normed = (scaled * lax.rsqrt(mean_square + EPS) * gain).astype(jnp.bfloat16)
    mixing = None
    for j in range(IN_CHUNKS):
        in_loads[j].wait()
        part = jnp.dot(
            normed[:, j * depth : (j + 1) * depth],
            w_in_v[pl.ds(j * depth, depth), :],
            preferred_element_type=jnp.float32,
        )
        mixing = part if mixing is None else mixing + part
    mixing = mixing.astype(jnp.bfloat16)
    for g in range(plan.groups):
        for s in range(plan.seqs):
            x_send[g * plan.seqs + s] = mixing[s * plan.here : (s + 1) * plan.here, g * G : (g + 1) * G]

    pl.semaphore_wait(barrier, plan.devices - 1)

    def x_copy(source, target):
        return pltpu.make_async_remote_copy(
            src_ref=x_send.at[lax.rem(target, plan.units)],
            dst_ref=x_recv.at[source],
            send_sem=x_send_sem.at[target],
            recv_sem=x_recv_sem.at[source],
            device_id=place(target),
            device_id_type=MESH,
        )

    for mask in range(plan.devices - 1, 0, -1):
        x_copy(me, partner(mask)).start()
    x_recv[me] = x_send[unit]
    table_load.wait()
    channel_load.wait()

    def x_wait(i, carry):
        x_copy(lax.rem(me + i, plan.devices), me).wait_recv()
        return carry

    lax.fori_loop(1, plan.devices, x_wait, 0)
    values = x_recv[...].reshape(plan.length, G)
    turned = jnp.dot(table_v[...], values, preferred_element_type=jnp.float32).astype(jnp.bfloat16)
    owned = plan.length // plan.halves
    both = jnp.concatenate([turned[:owned], turned[owned:]], axis=1)
    spectrum = jnp.dot(both, channel_v[...], preferred_element_type=jnp.float32).astype(jnp.bfloat16)
    s_send[...] = spectrum.reshape(s_send.shape)

    def s_copy(source, target):
        return pltpu.make_async_remote_copy(
            src_ref=s_send.at[target],
            dst_ref=s_recv.at[source],
            send_sem=s_send_sem.at[target],
            recv_sem=s_recv_sem.at[source],
            device_id=place(half * plan.units + target),
            device_id_type=MESH,
        )

    for mask in range(plan.units - 1, 0, -1):
        s_copy(unit, lax.rem(partner(mask), plan.units)).start()
    s_recv[unit] = s_send[unit]
    out_load.wait()

    def s_wait(i, carry):
        s_copy(lax.rem(unit + i, plan.units), unit).wait_recv()
        return carry

    lax.fori_loop(1, plan.units, s_wait, 0)
    mixed = jnp.concatenate(
        [
            jnp.concatenate([s_recv[g * plan.seqs + s] for s in range(plan.seqs)], axis=0)
            for g in range(plan.groups)
        ],
        axis=1,
    )
    for j in range(OUT_CHUNKS):
        piece = jnp.dot(
            mixed, w_out_v[:, pl.ds(j * span, span)], preferred_element_type=jnp.float32
        )
        for s in range(plan.seqs):
            for q in range(plan.q2):
                start = (s * plan.q2 + q) * plan.q1
                out_ref[s, q, :, pl.ds(j * span, span)] = piece[start : start + plan.q1].astype(jnp.bfloat16)

    def x_sent(i, carry):
        x_copy(me, lax.rem(me + i, plan.devices)).wait_send()
        return carry

    def s_sent(i, carry):
        s_copy(unit, lax.rem(unit + i, plan.units)).wait_send()
        return carry

    lax.fori_loop(1, plan.devices, x_sent, 0)
    lax.fori_loop(1, plan.units, s_sent, 0)


def kernel_body(plan, tokens, norm_gain, w_mix_in, w_mix_out):
    table, channel = plan.tables()
    bf16 = jnp.bfloat16
    dma = pltpu.SemaphoreType.DMA
    return pl.pallas_call(
        functools.partial(mix_kernel, plan),
        out_shape=jax.ShapeDtypeStruct((plan.seqs, plan.q2, plan.q1, plan.width), bf16),
        in_specs=[pl.BlockSpec(memory_space=pltpu.HBM)] * 6,
        out_specs=pl.BlockSpec(memory_space=pltpu.VMEM),
        scratch_shapes=[
            pltpu.VMEM(tokens.shape, bf16),
            pltpu.VMEM(norm_gain.shape, bf16),
            pltpu.VMEM(w_mix_in.shape, bf16),
            pltpu.VMEM(w_mix_out.shape, bf16),
            pltpu.VMEM(table.shape[1:], bf16),
            pltpu.VMEM(channel.shape, bf16),
            pltpu.VMEM((plan.seqs * plan.here, plan.width), jnp.float32),
            pltpu.VMEM((plan.units, plan.here, G), bf16),
            pltpu.VMEM((plan.devices, plan.here, G), bf16),
            pltpu.VMEM((plan.units, plan.q2 * plan.q1, G), bf16),
            pltpu.VMEM((plan.units, plan.q2 * plan.q1, G), bf16),
            dma((4,)),
            dma((IN_CHUNKS,)),
            dma((OUT_CHUNKS,)),
            dma((plan.devices,)),
            dma((plan.devices,)),
            dma((plan.units,)),
            dma((plan.units,)),
        ],
        compiler_params=pltpu.CompilerParams(
            collective_id=0, has_side_effects=True, vmem_limit_bytes=VMEM_BYTES
        ),
    )(*[
        pltpu.with_memory_space_constraint(x, pltpu.HBM)
        for x in (tokens, norm_gain, w_mix_in, w_mix_out, table, channel)
    ])


def solution(mesh):
    placed = (P(None, "row", "col", None), P(), P(), P())

    def run(tokens, norm_gain, w_mix_in, w_mix_out):
        plan = Plan(mesh, tokens.shape, w_mix_in.shape[1])
        body = functools.partial(kernel_body, plan) if plan.fits() else staged_body
        return jax.shard_map(
            body, mesh=mesh, in_specs=placed, out_specs=P(None, "row", "col", None), check_vma=False
        )(tokens, norm_gain, w_mix_in, w_mix_out)

    return run
```

```python
import functools
import math

import jax
import jax.numpy as jnp
import numpy as np
from jax import lax
from jax.experimental import pallas as pl
from jax.experimental.pallas import tpu as pltpu
from jax.sharding import PartitionSpec as P

MESH = pl.DeviceIdType.MESH

G = 128


EPS = 1e-06
HIGHEST = lax.Precision.HIGHEST


def as_sent(x):

    def short(part):
        return part.astype(jnp.bfloat16) if part.dtype == jnp.float32 else part

    return jax.tree.map(short, x)


def phase_table(count_first, count_second, period, first_start):
    first_index = lax.iota(jnp.int32, count_first) + first_start
    second_index = lax.iota(jnp.int32, count_second)
    turn_count = first_index[:, None] * second_index[None, :] % period
    phases = turn_count.astype(jnp.float32) * (2.0 * math.pi / period)
    return (jnp.cos(phases), jnp.sin(phases))


def packed_table(group_width):
    source = lax.iota(jnp.int32, group_width)
    column = lax.iota(jnp.int32, group_width)
    pair_index = column // 2
    frequency = jnp.where(column == 1, group_width // 2, pair_index)
    use_sine = (column % 2 == 1) & (pair_index > 0)
    turn_count = source[:, None] * frequency[None, :] % group_width
    phases = turn_count.astype(jnp.float32) * (2.0 * math.pi / group_width)
    return jnp.where(use_sine[None, :], jnp.sin(phases), jnp.cos(phases)) / math.sqrt(group_width)


def staged_body(tokens, norm_gain, w_mix_in, w_mix_out):
    seq_count, rows_here, cols_here, width = tokens.shape
    row_devices = lax.axis_size("row")
    col_devices = lax.axis_size("col")
    len_first = rows_here * row_devices
    len_second = cols_here * col_devices
    seq_length = len_first * len_second
    features = w_mix_in.shape[1]
    share = features // row_devices
    groups = features // G
    scaled = tokens.astype(jnp.float32)
    mean_square = jnp.mean(scaled * scaled, axis=-1, keepdims=True)
    normed = (scaled * lax.rsqrt(mean_square + EPS) * norm_gain.astype(jnp.float32)).astype(
        jnp.bfloat16
    )
    mixing_in = jnp.dot(
        normed.reshape(-1, width), w_mix_in, preferred_element_type=jnp.float32
    ).astype(jnp.bfloat16)
    grouped = mixing_in.astype(jnp.float32).reshape(seq_count, rows_here, cols_here, groups, G)
    first_cos, first_sin = phase_table(len_first, len_first, len_first, 0)
    first_cos = first_cos / math.sqrt(len_first)
    first_sin = first_sin / math.sqrt(len_first)
    col_start = lax.axis_index("col") * cols_here
    twist_cos, twist_sin = phase_table(cols_here, len_first, seq_length, col_start)
    twist_cos = twist_cos[None, :, None, :]
    twist_sin = twist_sin[None, :, None, :]
    packed = jnp.einsum("sabgc,cm->sabgm", grouped, packed_table(G), precision=HIGHEST)
    packed = packed.reshape(seq_count, rows_here, cols_here, features)
    turned = jnp.transpose(
        lax.all_to_all(
            packed.astype(jnp.bfloat16), "row", split_axis=3, concat_axis=1, tiled=True
        ).astype(packed.dtype),
        (0, 2, 3, 1),
    )
    real_out = jnp.einsum("njft,tk->njfk", turned, first_cos, precision=HIGHEST)
    imag_out = -jnp.einsum("njft,tk->njfk", turned, first_sin, precision=HIGHEST)
    spec_real = real_out * twist_cos + imag_out * twist_sin
    spec_imag = imag_out * twist_cos - real_out * twist_sin
    second_cos, second_sin = phase_table(len_second, len_second, len_second, 0)
    second_cos = second_cos / math.sqrt(len_second)
    second_sin = second_sin / math.sqrt(len_second)
    row_start = lax.axis_index("row") * share
    pair_global = row_start // 2 + lax.iota(jnp.int32, share // 2)
    head_pair = (pair_global % (G // 2) == 0)[:, None]
    real_in = lax.all_to_all(
        as_sent(spec_real), "col", split_axis=3, concat_axis=1, tiled=True
    ).astype(spec_real.dtype)
    imag_in = lax.all_to_all(
        as_sent(spec_imag), "col", split_axis=3, concat_axis=1, tiled=True
    ).astype(spec_imag.dtype)
    real_turned = jnp.transpose(real_in, (0, 3, 2, 1))
    imag_turned = jnp.transpose(imag_in, (0, 3, 2, 1))
    real_out = jnp.einsum("nqft,tk->nqfk", real_turned, second_cos, precision=HIGHEST) + jnp.einsum(
        "nqft,tk->nqfk", imag_turned, second_sin, precision=HIGHEST
    )
    imag_out = jnp.einsum("nqft,tk->nqfk", imag_turned, second_cos, precision=HIGHEST) - jnp.einsum(
        "nqft,tk->nqfk", real_turned, second_sin, precision=HIGHEST
    )
    out_shape = real_out.shape
    pair_shape = out_shape[:2] + (share // 2, 2, out_shape[3])
    real_pairs = real_out.reshape(pair_shape)
    imag_pairs = imag_out.reshape(pair_shape)
    even_real = real_pairs[:, :, :, 0, :]
    odd_real = real_pairs[:, :, :, 1, :]
    odd_imag = imag_pairs[:, :, :, 1, :]
    low_freq = jnp.where(head_pair, even_real, even_real + odd_imag)
    high_freq = jnp.where(head_pair, odd_real, even_real - odd_imag)
    joined = jnp.stack([low_freq, high_freq], axis=3).reshape(out_shape).astype(jnp.bfloat16)
    mixed = jnp.transpose(joined, (0, 3, 1, 2))
    piece = lax.all_to_all(mixed, "row", split_axis=1, concat_axis=3, tiled=True)
    paired = piece.reshape(piece.shape[:-1] + (groups, G // 2, 2))
    low_freq = paired[..., 0]
    high_freq = paired[..., 1]
    natural = jnp.concatenate(
        [low_freq, high_freq[..., :1], jnp.flip(high_freq[..., 1:], axis=-1)], axis=-1
    )
    project_piece = natural.reshape(piece.shape)
    flat = project_piece.reshape(-1, features)
    output = jnp.dot(flat, w_mix_out, preferred_element_type=jnp.float32).astype(jnp.bfloat16)
    return output.reshape(project_piece.shape[:-1] + (width,))


class Plan:
    def __init__(self, mesh, tokens_shape, features):
        self.rows, self.cols = mesh.shape["row"], mesh.shape["col"]
        self.devices = self.rows * self.cols
        self.seqs, len_first, len_second, self.width = tokens_shape
        self.len_first, self.len_second = len_first, len_second
        self.features = features
        self.groups = features // G
        self.t1, self.t2 = len_first // self.rows, len_second // self.cols
        self.here = self.t1 * self.t2
        self.length = len_first * len_second
        self.q2, self.q1 = len_second // self.rows, len_first // self.cols

    def fits(self):
        if self.features % G or self.devices != 4 * self.groups or self.length > 1024:
            return False
        if self.devices & (self.devices - 1) or self.rows % 2 or self.cols % 2:
            return False
        if self.len_second % self.rows or self.len_first % self.cols:
            return False
        if self.here % 16 or self.q1 % 8 or self.q2 * self.q1 % 16:
            return False
        self.half_rows, self.side_cols = self.rows // 2, self.cols // 2
        self.span = self.devices // 2
        return True

    def tables(self):
        row, col, a, b = np.meshgrid(
            np.arange(self.rows), np.arange(self.cols), np.arange(self.t1), np.arange(self.t2), indexing="ij"
        )
        time = (row * self.t1 + a) * self.len_second + col * self.t2 + b
        time = np.stack([part.reshape(-1) for part in np.split(time, 2, axis=1)])
        row, col, a, b = np.meshgrid(
            np.arange(self.rows), np.arange(self.cols), np.arange(self.q2), np.arange(self.q1), indexing="ij"
        )
        freq = (col * self.q1 + b + self.len_first * (row * self.q2 + a)).reshape(2, -1)
        turn = 2.0 * np.pi / self.length * (freq[:, None, :, None] * time[None, :, None, :] % self.length)
        scale = 1.0 / math.sqrt(self.length * G)
        first = 2.0 ** round(math.log2(scale) / 2)
        position = np.concatenate([np.cos(turn), np.sin(turn)], axis=2) * first
        channel = np.arange(G)
        turn = 2.0 * np.pi / G * (channel[:, None] * channel[None, :] % G)
        channel = np.concatenate([np.cos(turn), -np.sin(turn)], axis=0) * (scale / first)
        return jnp.asarray(position, jnp.bfloat16), jnp.asarray(channel, jnp.bfloat16)


VMEM_BYTES = 16 * 1024 * 1024
IN_CHUNKS = 4
OUT_CHUNKS = 4


def mix_kernel(
    plan, tokens_hbm, gain_hbm, w_in_hbm, w_out_hbm, table_hbm, channel_hbm, out_ref,
    tokens_v, gain_v, w_in_v, w_out_v, table_v, channel_v, flat_v,
    x_send, x_recv, s_send, s_recv,
    load_sem, in_sem, out_sem, x_send_sem, x_recv_sem, s_send_sem, s_recv_sem,
):
    row, col = lax.axis_index("row"), lax.axis_index("col")
    me = row * plan.cols + col
    half, side = row // plan.half_rows, col // plan.side_cols
    in_half = lax.rem(me, plan.span)
    group_of = lambda d: lax.rem(d // plan.cols, plan.half_rows) * plan.side_cols + lax.rem(d, plan.side_cols)
    in_side = lambda d: d // plan.cols * plan.side_cols + lax.rem(d, plan.side_cols)
    x_masks = [m for m in range(plan.devices - 1, 0, -1) if not m & plan.side_cols]
    s_masks = list(range(plan.span - 1, 0, -1))
    place = lambda d: {"row": d // plan.cols, "col": lax.rem(d, plan.cols)}

    barrier = pltpu.get_barrier_semaphore()

    flips = []
    bit = 1
    while bit < plan.devices:
        flips.append((bit, bit * (1 - 2 * lax.rem(me // bit, 2))))
        bit *= 2

    def partner(mask):
        return me + sum(step for bit, step in flips if mask & bit)

    token_load = pltpu.make_async_copy(tokens_hbm, tokens_v, load_sem.at[0])
    gain_load = pltpu.make_async_copy(gain_hbm, gain_v, load_sem.at[1])
    table_load = pltpu.make_async_copy(table_hbm.at[half, side], table_v, load_sem.at[2])
    channel_load = pltpu.make_async_copy(channel_hbm, channel_v, load_sem.at[3])
    depth = plan.width // IN_CHUNKS
    in_loads = [
        pltpu.make_async_copy(
            w_in_hbm.at[pl.ds(j * depth, depth)], w_in_v.at[pl.ds(j * depth, depth)], in_sem.at[j]
        )
        for j in range(IN_CHUNKS)
    ]
    span = plan.width // OUT_CHUNKS
    out_load = pltpu.make_async_copy(w_out_hbm, w_out_v, out_sem.at[0])
    token_load.start()
    gain_load.start()
    for load in in_loads:
        load.start()
    peers = [m for m in range(plan.devices - 1, 0, -1) if m in x_masks or m in s_masks]
    for mask in peers:
        pl.semaphore_signal(barrier, inc=1, device_id=place(partner(mask)), device_id_type=MESH)

    token_load.wait()
    for s in range(plan.seqs):
        for a in range(plan.t1):
            flat_v[pl.ds((s * plan.t1 + a) * plan.t2, plan.t2), :] = tokens_v[s, a].astype(jnp.float32)
    scaled = flat_v[...]
    mean_square = jnp.mean(scaled * scaled, axis=-1, keepdims=True)
    gain_load.wait()
    gain = gain_v[...].astype(jnp.float32).reshape(1, plan.width)
    normed = (scaled * lax.rsqrt(mean_square + EPS) * gain).astype(jnp.bfloat16)
    mixing = None
    for j in range(IN_CHUNKS):
        in_loads[j].wait()
        part = jnp.dot(
            normed[:, j * depth : (j + 1) * depth],
            w_in_v[pl.ds(j * depth, depth), :],
            preferred_element_type=jnp.float32,
        )
        mixing = part if mixing is None else mixing + part
    mixing = mixing.astype(jnp.bfloat16)
    for g in range(plan.groups):
        x_send[g] = mixing[:, g * G : (g + 1) * G]
    table_load.start()
    channel_load.start()
    out_load.start()

    pl.semaphore_wait(barrier, len(peers))

    def x_copy(source, target):
        return pltpu.make_async_remote_copy(
            src_ref=x_send.at[group_of(target)],
            dst_ref=x_recv.at[in_side(source)],
            send_sem=x_send_sem.at[in_side(target)],
            recv_sem=x_recv_sem.at[in_side(source)],
            device_id=place(target),
            device_id_type=MESH,
        )

    for mask in x_masks:
        x_copy(me, partner(mask)).start()
    x_recv[in_side(me)] = x_send[group_of(me)]
    table_load.wait()
    channel_load.wait()
    for mask in reversed(x_masks):
        x_copy(partner(mask), me).wait_recv()
    values = jnp.concatenate(
        [
            x_recv[:, pl.ds(s * plan.here, plan.here), :].reshape(plan.span * plan.here, G)
            for s in range(plan.seqs)
        ],
        axis=1,
    )
    turned = jnp.dot(table_v[...], values, preferred_element_type=jnp.float32).astype(jnp.bfloat16)
    owned = plan.length // 2
    piece = plan.q2 * plan.q1
    for s in range(plan.seqs):
        lanes = slice(s * G, (s + 1) * G)
        both = jnp.concatenate([turned[:owned, lanes], turned[owned:, lanes]], axis=1)
        spectrum = jnp.dot(both, channel_v[...], preferred_element_type=jnp.float32)
        s_send[:, pl.ds(s * piece, piece), :] = spectrum.astype(jnp.bfloat16).reshape(plan.span, piece, G)

    def s_copy(source, target):
        return pltpu.make_async_remote_copy(
            src_ref=s_send.at[target],
            dst_ref=s_recv.at[source],
            send_sem=s_send_sem.at[target],
            recv_sem=s_recv_sem.at[source],
            device_id=place(half * plan.span + target),
            device_id_type=MESH,
        )

    for mask in s_masks:
        s_copy(in_half, lax.rem(partner(mask), plan.span)).start()
    s_recv[in_half] = s_send[in_half]
    out_load.wait()
    for mask in reversed(s_masks):
        s_copy(lax.rem(partner(mask), plan.span), in_half).wait_recv()

    def sides_sum(g):
        first = g // plan.side_cols * plan.cols + g % plan.side_cols
        total = s_recv[first].astype(jnp.float32) + s_recv[first + plan.side_cols].astype(jnp.float32)
        return total.astype(jnp.bfloat16)

    mixed = jnp.concatenate([sides_sum(g) for g in range(plan.groups)], axis=1)
    for j in range(OUT_CHUNKS):
        piece = jnp.dot(
            mixed, w_out_v[:, pl.ds(j * span, span)], preferred_element_type=jnp.float32
        )
        for s in range(plan.seqs):
            for q in range(plan.q2):
                start = (s * plan.q2 + q) * plan.q1
                out_ref[s, q, :, pl.ds(j * span, span)] = piece[start : start + plan.q1].astype(jnp.bfloat16)

    for mask in x_masks:
        x_copy(me, partner(mask)).wait_send()
    for mask in s_masks:
        s_copy(in_half, lax.rem(partner(mask), plan.span)).wait_send()


def kernel_body(plan, tokens, norm_gain, w_mix_in, w_mix_out):
    table, channel = plan.tables()
    bf16 = jnp.bfloat16
    dma = pltpu.SemaphoreType.DMA
    return pl.pallas_call(
        functools.partial(mix_kernel, plan),
        out_shape=jax.ShapeDtypeStruct((plan.seqs, plan.q2, plan.q1, plan.width), bf16),
        in_specs=[pl.BlockSpec(memory_space=pltpu.HBM)] * 6,
        out_specs=pl.BlockSpec(memory_space=pltpu.VMEM),
        scratch_shapes=[
            pltpu.VMEM(tokens.shape, bf16),
            pltpu.VMEM(norm_gain.shape, bf16),
            pltpu.VMEM(w_mix_in.shape, bf16),
            pltpu.VMEM(w_mix_out.shape, bf16),
            pltpu.VMEM(table.shape[2:], bf16),
            pltpu.VMEM(channel.shape, bf16),
            pltpu.VMEM((plan.seqs * plan.here, plan.width), jnp.float32),
            pltpu.VMEM((plan.groups, plan.seqs * plan.here, G), bf16),
            pltpu.VMEM((plan.span, plan.seqs * plan.here, G), bf16),
            pltpu.VMEM((plan.span, plan.seqs * plan.q2 * plan.q1, G), bf16),
            pltpu.VMEM((plan.span, plan.seqs * plan.q2 * plan.q1, G), bf16),
            dma((4,)),
            dma((IN_CHUNKS,)),
            dma((1,)),
            dma((plan.span,)),
            dma((plan.span,)),
            dma((plan.span,)),
            dma((plan.span,)),
        ],
        compiler_params=pltpu.CompilerParams(
            collective_id=0, has_side_effects=True, vmem_limit_bytes=VMEM_BYTES
        ),
    )(*[
        pltpu.with_memory_space_constraint(x, pltpu.HBM)
        for x in (tokens, norm_gain, w_mix_in, w_mix_out, table, channel)
    ])


def solution(mesh):
    placed = (P(None, "row", "col", None), P(), P(), P())

    def run(tokens, norm_gain, w_mix_in, w_mix_out):
        plan = Plan(mesh, tokens.shape, w_mix_in.shape[1])
        body = functools.partial(kernel_body, plan) if plan.fits() else staged_body
        return jax.shard_map(
            body, mesh=mesh, in_specs=placed, out_specs=P(None, "row", "col", None), check_vma=False
        )(tokens, norm_gain, w_mix_in, w_mix_out)

    return run
```

```python
import functools
import math

import jax
import jax.numpy as jnp
import numpy as np
from jax import lax
from jax.experimental import pallas as pl
from jax.experimental.pallas import tpu as pltpu
from jax.sharding import PartitionSpec as P

MESH = pl.DeviceIdType.MESH

G = 128


EPS = 1e-06
HIGHEST = lax.Precision.HIGHEST


def as_sent(x):

    def short(part):
        return part.astype(jnp.bfloat16) if part.dtype == jnp.float32 else part

    return jax.tree.map(short, x)


def phase_table(count_first, count_second, period, first_start):
    first_index = lax.iota(jnp.int32, count_first) + first_start
    second_index = lax.iota(jnp.int32, count_second)
    turn_count = first_index[:, None] * second_index[None, :] % period
    phases = turn_count.astype(jnp.float32) * (2.0 * math.pi / period)
    return (jnp.cos(phases), jnp.sin(phases))


def packed_table(group_width):
    source = lax.iota(jnp.int32, group_width)
    column = lax.iota(jnp.int32, group_width)
    pair_index = column // 2
    frequency = jnp.where(column == 1, group_width // 2, pair_index)
    use_sine = (column % 2 == 1) & (pair_index > 0)
    turn_count = source[:, None] * frequency[None, :] % group_width
    phases = turn_count.astype(jnp.float32) * (2.0 * math.pi / group_width)
    return jnp.where(use_sine[None, :], jnp.sin(phases), jnp.cos(phases)) / math.sqrt(group_width)


def staged_body(tokens, norm_gain, w_mix_in, w_mix_out):
    seq_count, rows_here, cols_here, width = tokens.shape
    row_devices = lax.axis_size("row")
    col_devices = lax.axis_size("col")
    len_first = rows_here * row_devices
    len_second = cols_here * col_devices
    seq_length = len_first * len_second
    features = w_mix_in.shape[1]
    share = features // row_devices
    groups = features // G
    scaled = tokens.astype(jnp.float32)
    mean_square = jnp.mean(scaled * scaled, axis=-1, keepdims=True)
    normed = (scaled * lax.rsqrt(mean_square + EPS) * norm_gain.astype(jnp.float32)).astype(
        jnp.bfloat16
    )
    mixing_in = jnp.dot(
        normed.reshape(-1, width), w_mix_in, preferred_element_type=jnp.float32
    ).astype(jnp.bfloat16)
    grouped = mixing_in.astype(jnp.float32).reshape(seq_count, rows_here, cols_here, groups, G)
    first_cos, first_sin = phase_table(len_first, len_first, len_first, 0)
    first_cos = first_cos / math.sqrt(len_first)
    first_sin = first_sin / math.sqrt(len_first)
    col_start = lax.axis_index("col") * cols_here
    twist_cos, twist_sin = phase_table(cols_here, len_first, seq_length, col_start)
    twist_cos = twist_cos[None, :, None, :]
    twist_sin = twist_sin[None, :, None, :]
    packed = jnp.einsum("sabgc,cm->sabgm", grouped, packed_table(G), precision=HIGHEST)
    packed = packed.reshape(seq_count, rows_here, cols_here, features)
    turned = jnp.transpose(
        lax.all_to_all(
            packed.astype(jnp.bfloat16), "row", split_axis=3, concat_axis=1, tiled=True
        ).astype(packed.dtype),
        (0, 2, 3, 1),
    )
    real_out = jnp.einsum("njft,tk->njfk", turned, first_cos, precision=HIGHEST)
    imag_out = -jnp.einsum("njft,tk->njfk", turned, first_sin, precision=HIGHEST)
    spec_real = real_out * twist_cos + imag_out * twist_sin
    spec_imag = imag_out * twist_cos - real_out * twist_sin
    second_cos, second_sin = phase_table(len_second, len_second, len_second, 0)
    second_cos = second_cos / math.sqrt(len_second)
    second_sin = second_sin / math.sqrt(len_second)
    row_start = lax.axis_index("row") * share
    pair_global = row_start // 2 + lax.iota(jnp.int32, share // 2)
    head_pair = (pair_global % (G // 2) == 0)[:, None]
    real_in = lax.all_to_all(
        as_sent(spec_real), "col", split_axis=3, concat_axis=1, tiled=True
    ).astype(spec_real.dtype)
    imag_in = lax.all_to_all(
        as_sent(spec_imag), "col", split_axis=3, concat_axis=1, tiled=True
    ).astype(spec_imag.dtype)
    real_turned = jnp.transpose(real_in, (0, 3, 2, 1))
    imag_turned = jnp.transpose(imag_in, (0, 3, 2, 1))
    real_out = jnp.einsum("nqft,tk->nqfk", real_turned, second_cos, precision=HIGHEST) + jnp.einsum(
        "nqft,tk->nqfk", imag_turned, second_sin, precision=HIGHEST
    )
    imag_out = jnp.einsum("nqft,tk->nqfk", imag_turned, second_cos, precision=HIGHEST) - jnp.einsum(
        "nqft,tk->nqfk", real_turned, second_sin, precision=HIGHEST
    )
    out_shape = real_out.shape
    pair_shape = out_shape[:2] + (share // 2, 2, out_shape[3])
    real_pairs = real_out.reshape(pair_shape)
    imag_pairs = imag_out.reshape(pair_shape)
    even_real = real_pairs[:, :, :, 0, :]
    odd_real = real_pairs[:, :, :, 1, :]
    odd_imag = imag_pairs[:, :, :, 1, :]
    low_freq = jnp.where(head_pair, even_real, even_real + odd_imag)
    high_freq = jnp.where(head_pair, odd_real, even_real - odd_imag)
    joined = jnp.stack([low_freq, high_freq], axis=3).reshape(out_shape).astype(jnp.bfloat16)
    mixed = jnp.transpose(joined, (0, 3, 1, 2))
    piece = lax.all_to_all(mixed, "row", split_axis=1, concat_axis=3, tiled=True)
    paired = piece.reshape(piece.shape[:-1] + (groups, G // 2, 2))
    low_freq = paired[..., 0]
    high_freq = paired[..., 1]
    natural = jnp.concatenate(
        [low_freq, high_freq[..., :1], jnp.flip(high_freq[..., 1:], axis=-1)], axis=-1
    )
    project_piece = natural.reshape(piece.shape)
    flat = project_piece.reshape(-1, features)
    output = jnp.dot(flat, w_mix_out, preferred_element_type=jnp.float32).astype(jnp.bfloat16)
    return output.reshape(project_piece.shape[:-1] + (width,))


class Plan:
    def __init__(self, mesh, tokens_shape, features):
        self.rows, self.cols = mesh.shape["row"], mesh.shape["col"]
        self.devices = self.rows * self.cols
        self.seqs, len_first, len_second, self.width = tokens_shape
        self.len_first, self.len_second = len_first, len_second
        self.features = features
        self.groups = features // G
        self.t1, self.t2 = len_first // self.rows, len_second // self.cols
        self.here = self.t1 * self.t2
        self.length = len_first * len_second
        self.q2, self.q1 = len_second // self.rows, len_first // self.cols

    def fits(self):
        if self.features % G or self.devices != 4 * self.groups or self.length > 1024:
            return False
        if self.devices & (self.devices - 1) or self.rows % 2 or self.cols % 2:
            return False
        if self.len_second % self.rows or self.len_first % self.cols:
            return False
        if self.here % 16 or self.q1 % 8 or self.q2 * self.q1 % 16:
            return False
        self.half_rows, self.side_cols = self.rows // 2, self.cols // 2
        self.span = self.devices // 2
        return True

    def tables(self):
        row, col, a, b = np.meshgrid(
            np.arange(self.rows), np.arange(self.cols), np.arange(self.t1), np.arange(self.t2), indexing="ij"
        )
        time = (row * self.t1 + a) * self.len_second + col * self.t2 + b
        time = np.stack([part.reshape(-1) for part in np.split(time, 2, axis=1)])
        row, col, a, b = np.meshgrid(
            np.arange(self.rows), np.arange(self.cols), np.arange(self.q2), np.arange(self.q1), indexing="ij"
        )
        freq = (col * self.q1 + b + self.len_first * (row * self.q2 + a)).reshape(2, -1)
        turn = 2.0 * np.pi / self.length * (freq[:, None, :, None] * time[None, :, None, :] % self.length)
        scale = 1.0 / math.sqrt(self.length * G)
        first = 2.0 ** round(math.log2(scale) / 2)
        position = np.concatenate([np.cos(turn), np.sin(turn)], axis=2) * first
        channel = np.arange(G)
        turn = 2.0 * np.pi / G * (channel[:, None] * channel[None, :] % G)
        channel = np.concatenate([np.cos(turn), -np.sin(turn)], axis=0) * (scale / first)
        return jnp.asarray(position, jnp.bfloat16), jnp.asarray(channel, jnp.bfloat16)


VMEM_BYTES = 16 * 1024 * 1024
IN_CHUNKS = 4
OUT_CHUNKS = 4


def mix_kernel(
    plan, tokens_hbm, gain_hbm, w_in_hbm, w_out_hbm, table_hbm, channel_hbm, out_ref,
    tokens_v, gain_v, w_in_v, w_out_v, table_v, channel_v, flat_v,
    x_send, x_recv, s_send, s_recv,
    load_sem, in_sem, out_sem, x_send_sem, x_recv_sem, s_send_sem, s_recv_sem,
):
    row, col = lax.axis_index("row"), lax.axis_index("col")
    me = row * plan.cols + col
    half, side = row // plan.half_rows, col // plan.side_cols
    in_half = lax.rem(me, plan.span)
    group_of = lambda d: lax.rem(d // plan.cols, plan.half_rows) * plan.side_cols + lax.rem(d, plan.side_cols)
    in_side = lambda d: d // plan.cols * plan.side_cols + lax.rem(d, plan.side_cols)
    x_masks = [m for m in range(plan.devices - 1, 0, -1) if not m & plan.side_cols]
    s_masks = list(range(plan.span - 1, 0, -1))
    place = lambda d: {"row": d // plan.cols, "col": lax.rem(d, plan.cols)}

    barrier = pltpu.get_barrier_semaphore()

    flips = []
    bit = 1
    while bit < plan.devices:
        flips.append((bit, bit * (1 - 2 * lax.rem(me // bit, 2))))
        bit *= 2

    def partner(mask):
        return me + sum(step for bit, step in flips if mask & bit)

    token_load = pltpu.make_async_copy(tokens_hbm, tokens_v, load_sem.at[0])
    gain_load = pltpu.make_async_copy(gain_hbm, gain_v, load_sem.at[1])
    table_load = pltpu.make_async_copy(table_hbm.at[half, side], table_v, load_sem.at[2])
    channel_load = pltpu.make_async_copy(channel_hbm, channel_v, load_sem.at[3])
    depth = plan.width // IN_CHUNKS
    in_loads = [
        pltpu.make_async_copy(
            w_in_hbm.at[pl.ds(j * depth, depth)], w_in_v.at[pl.ds(j * depth, depth)], in_sem.at[j]
        )
        for j in range(IN_CHUNKS)
    ]
    span = plan.width // OUT_CHUNKS
    out_load = pltpu.make_async_copy(w_out_hbm, w_out_v, out_sem.at[0])
    token_load.start()
    gain_load.start()
    for load in in_loads:
        load.start()
    peers = [m for m in range(plan.devices - 1, 0, -1) if m in x_masks or m in s_masks]
    for mask in peers:
        pl.semaphore_signal(barrier, inc=1, device_id=place(partner(mask)), device_id_type=MESH)

    token_load.wait()
    for s in range(plan.seqs):
        for a in range(plan.t1):
            flat_v[pl.ds((s * plan.t1 + a) * plan.t2, plan.t2), :] = tokens_v[s, a].astype(jnp.float32)
    scaled = flat_v[...]
    mean_square = jnp.mean(scaled * scaled, axis=-1, keepdims=True)
    gain_load.wait()
    gain = gain_v[...].astype(jnp.float32).reshape(1, plan.width)
    normed = (scaled * lax.rsqrt(mean_square + EPS) * gain).astype(jnp.bfloat16)
    mixing = None
    for j in range(IN_CHUNKS):
        in_loads[j].wait()
        part = jnp.dot(
            normed[:, j * depth : (j + 1) * depth],
            w_in_v[pl.ds(j * depth, depth), :],
            preferred_element_type=jnp.float32,
        )
        mixing = part if mixing is None else mixing + part
    mixing = mixing.astype(jnp.bfloat16)
    for g in range(plan.groups):
        x_send[g] = mixing[:, g * G : (g + 1) * G]
    table_load.start()
    channel_load.start()
    out_load.start()

    pl.semaphore_wait(barrier, len(peers))

    def x_copy(source, target):
        return pltpu.make_async_remote_copy(
            src_ref=x_send.at[group_of(target)],
            dst_ref=x_recv.at[in_side(source)],
            send_sem=x_send_sem.at[in_side(target)],
            recv_sem=x_recv_sem.at[in_side(source)],
            device_id=place(target),
            device_id_type=MESH,
        )

    for to_half in range(2):
        for mask in [m for m in x_masks if m < plan.span]:
            x_copy(me, to_half * plan.span + lax.rem(partner(mask), plan.span)).start()

        @pl.when(half != to_half)
        def _():
            x_copy(me, to_half * plan.span + in_half).start()

    x_recv[in_side(me)] = x_send[group_of(me)]
    table_load.wait()
    channel_load.wait()
    for mask in reversed(x_masks):
        x_copy(partner(mask), me).wait_recv()
    values = jnp.concatenate(
        [
            x_recv[:, pl.ds(s * plan.here, plan.here), :].reshape(plan.span * plan.here, G)
            for s in range(plan.seqs)
        ],
        axis=1,
    )
    turned = jnp.dot(table_v[...], values, preferred_element_type=jnp.float32).astype(jnp.bfloat16)
    owned = plan.length // 2
    piece = plan.q2 * plan.q1
    for s in range(plan.seqs):
        lanes = slice(s * G, (s + 1) * G)
        both = jnp.concatenate([turned[:owned, lanes], turned[owned:, lanes]], axis=1)
        spectrum = jnp.dot(both, channel_v[...], preferred_element_type=jnp.float32)
        s_send[:, pl.ds(s * piece, piece), :] = spectrum.astype(jnp.bfloat16).reshape(plan.span, piece, G)

    def s_copy(source, target):
        return pltpu.make_async_remote_copy(
            src_ref=s_send.at[target],
            dst_ref=s_recv.at[source],
            send_sem=s_send_sem.at[target],
            recv_sem=s_recv_sem.at[source],
            device_id=place(half * plan.span + target),
            device_id_type=MESH,
        )

    for target in range(plan.span):

        @pl.when(in_half != target)
        def _(target=target):
            s_copy(in_half, target).start()

    s_recv[in_half] = s_send[in_half]
    out_load.wait()
    for mask in reversed(s_masks):
        s_copy(lax.rem(partner(mask), plan.span), in_half).wait_recv()

    def sides_sum(g):
        first = g // plan.side_cols * plan.cols + g % plan.side_cols
        total = s_recv[first].astype(jnp.float32) + s_recv[first + plan.side_cols].astype(jnp.float32)
        return total.astype(jnp.bfloat16)

    mixed = jnp.concatenate([sides_sum(g) for g in range(plan.groups)], axis=1)
    for j in range(OUT_CHUNKS):
        piece = jnp.dot(
            mixed, w_out_v[:, pl.ds(j * span, span)], preferred_element_type=jnp.float32
        )
        for s in range(plan.seqs):
            for q in range(plan.q2):
                start = (s * plan.q2 + q) * plan.q1
                out_ref[s, q, :, pl.ds(j * span, span)] = piece[start : start + plan.q1].astype(jnp.bfloat16)

    for mask in x_masks:
        x_copy(me, partner(mask)).wait_send()
    for mask in s_masks:
        s_copy(in_half, lax.rem(partner(mask), plan.span)).wait_send()


def kernel_body(plan, tokens, norm_gain, w_mix_in, w_mix_out):
    table, channel = plan.tables()
    bf16 = jnp.bfloat16
    dma = pltpu.SemaphoreType.DMA
    return pl.pallas_call(
        functools.partial(mix_kernel, plan),
        out_shape=jax.ShapeDtypeStruct((plan.seqs, plan.q2, plan.q1, plan.width), bf16),
        in_specs=[pl.BlockSpec(memory_space=pltpu.HBM)] * 6,
        out_specs=pl.BlockSpec(memory_space=pltpu.VMEM),
        scratch_shapes=[
            pltpu.VMEM(tokens.shape, bf16),
            pltpu.VMEM(norm_gain.shape, bf16),
            pltpu.VMEM(w_mix_in.shape, bf16),
            pltpu.VMEM(w_mix_out.shape, bf16),
            pltpu.VMEM(table.shape[2:], bf16),
            pltpu.VMEM(channel.shape, bf16),
            pltpu.VMEM((plan.seqs * plan.here, plan.width), jnp.float32),
            pltpu.VMEM((plan.groups, plan.seqs * plan.here, G), bf16),
            pltpu.VMEM((plan.span, plan.seqs * plan.here, G), bf16),
            pltpu.VMEM((plan.span, plan.seqs * plan.q2 * plan.q1, G), bf16),
            pltpu.VMEM((plan.span, plan.seqs * plan.q2 * plan.q1, G), bf16),
            dma((4,)),
            dma((IN_CHUNKS,)),
            dma((1,)),
            dma((plan.span,)),
            dma((plan.span,)),
            dma((plan.span,)),
            dma((plan.span,)),
        ],
        compiler_params=pltpu.CompilerParams(
            collective_id=0, has_side_effects=True, vmem_limit_bytes=VMEM_BYTES
        ),
    )(*[
        pltpu.with_memory_space_constraint(x, pltpu.HBM)
        for x in (tokens, norm_gain, w_mix_in, w_mix_out, table, channel)
    ])


def solution(mesh):
    placed = (P(None, "row", "col", None), P(), P(), P())

    def run(tokens, norm_gain, w_mix_in, w_mix_out):
        plan = Plan(mesh, tokens.shape, w_mix_in.shape[1])
        body = functools.partial(kernel_body, plan) if plan.fits() else staged_body
        return jax.shard_map(
            body, mesh=mesh, in_specs=placed, out_specs=P(None, "row", "col", None), check_vma=False
        )(tokens, norm_gain, w_mix_in, w_mix_out)

    return run
```
